32 devices in a mesh: rep: 2 (over x), fs: 8 (over z, y), tp: 2 (over core).
Axes of the slice: x: 2, y: 2, z: 4, core: 2. Of those that a mesh axis runs over, the one named last changes fastest.
Arguments:
- tokens: bfloat16 [4096, 2048], P(('rep', 'fs', 'tp')), may hold values from -6 to 6
- mix_gain: float32 [2048], replicated, may hold values from 0.1 to 1.9
- conv_in_weight: bfloat16 [2048, 1024], P('fs', 'tp'), may hold values from -0.125 to 0.125
- gate_outer_weight: bfloat16 [2048, 1024], P('fs', 'tp'), may hold values from -0.125 to 0.125
- gate_inner_weight: bfloat16 [2048, 1024], P('fs', 'tp'), may hold values from -0.125 to 0.125
- conv_taps: float32 [3, 1024], P(None, 'tp'), may hold values from -3.5 to 3.5
- out_weight: bfloat16 [1024, 2048], P('tp', 'fs'), may hold values from -0.1875 to 0.1875
- ff_gain: float32 [2048], replicated, may hold values from 0.1 to 1.9
- up_weight: bfloat16 [2048, 8192], P('fs', 'tp'), may hold values from -0.125 to 0.125
- down_weight: bfloat16 [8192, 2048], P('tp', 'fs'), may hold values from -0.0625 to 0.0625
Outputs:
- layer_out: bfloat16 [4096, 2048], P(('rep', 'fs', 'tp'))
The draws below stay inside these ranges and needn't reach their ends.
All inputs are finite; a program needn't handle non-finite values.
Results may differ from the reference program's by a relative error of at most 0.023.
Values may be sent and summed in bfloat16 or wider, within the bound.
A program may use at most 128 MiB of HBM per device.

```python
import jax
import jax.numpy as jnp
from jax import lax

D = 2048
CONV = 1024
FF = 8192
TAPS = 3
SEQ = 256
TOKENS = 4096
CONV_DEV = 512
FF_DEV = 4096


def block_levels(own_key, extent, shards, least, largest):
    def one(dim, shards_of):
        draws = jax.random.uniform(jax.random.fold_in(jax.random.fold_in(own_key, 6), dim), (shards_of,), jnp.float32, least / len(shards), largest / len(shards))
        return jnp.repeat(jnp.exp(draws), extent[dim] // shards_of).reshape((-1,) + (1,) * (len(extent) - dim - 1))

    loudness = one(*shards[0])
    for cut in shards[1:]:
        loudness = loudness * one(*cut)
    return loudness


def noise(rng, extent, spread, bound, split=(), held_as=jnp.bfloat16):
    result = spread * jax.random.normal(rng, extent, jnp.float32)
    if split:
        result = result * block_levels(rng, extent, split, -0.22, 0.18)
    return jnp.clip(result, -bound, bound).astype(held_as)


def setup_inputs(seed: int = 0) -> dict:
    keys = jax.random.split(jax.random.key(seed), 11)
    tokens = noise(keys[0], (TOKENS, D), 1.0, 6.0, ((0, 32),))
    mix_gain = jnp.clip(1.0 + 0.18 * jax.random.normal(keys[1], (D,), jnp.float32), 0.1, 1.9)
    conv_in_weight = noise(keys[2], (D, CONV), D ** -0.5, 0.125, ((0, 8), (1, 2)))
    gate_outer_weight = noise(keys[3], (D, CONV), D ** -0.5, 0.125, ((0, 8), (1, 2)))
    gate_inner_weight = noise(keys[4], (D, CONV), D ** -0.5, 0.125, ((0, 8), (1, 2)))
    conv_taps = noise(keys[5], (TAPS, CONV), TAPS ** -0.5, 3.5, ((1, 2),), jnp.float32)
    out_weight = noise(keys[6], (CONV, D), CONV ** -0.5, 0.1875, ((0, 2), (1, 8)))
    ff_gain = jnp.clip(1.0 + 0.18 * jax.random.normal(keys[7], (D,), jnp.float32), 0.1, 1.9)
    up_weight = noise(keys[8], (D, FF), D ** -0.5, 0.125, ((0, 8), (1, 2)))
    down_weight = noise(keys[9], (FF, D), FF ** -0.5, 0.0625, ((0, 2), (1, 8)))
    return {"tokens": tokens, "mix_gain": mix_gain, "conv_in_weight": conv_in_weight, "gate_outer_weight": gate_outer_weight, "gate_inner_weight": gate_inner_weight, "conv_taps": conv_taps, "out_weight": out_weight, "ff_gain": ff_gain, "up_weight": up_weight, "down_weight": down_weight}


eps = 1e-06

def rms_scale(values, gain):
    widened = values.astype(jnp.float32)
    inverse = lax.rsqrt(lax.optimization_barrier(jnp.mean(widened * widened, axis=-1, keepdims=True)) + eps)
    return (widened * inverse * gain).astype(jnp.bfloat16)

def block_sum(activ, weight, width):
    blocks = activ.shape[1] // width

    def step(index, total):
        lefts = lax.dynamic_slice_in_dim(activ, index * width, width, 1)
        rights = lax.dynamic_slice_in_dim(weight, index * width, width, 0)
        rounded = jnp.dot(lefts, rights, preferred_element_type=jnp.float32).astype(jnp.bfloat16)
        rounded = lax.optimization_barrier(rounded)
        return total + rounded.astype(jnp.float32)
    initial = jnp.zeros((activ.shape[0], weight.shape[1]), jnp.float32)
    return lax.fori_loop(0, blocks, step, initial)

def reference(tokens, mix_gain, conv_in_weight, gate_outer_weight, gate_inner_weight, conv_taps, out_weight, ff_gain, up_weight, down_weight):
    normed = rms_scale(tokens, mix_gain)
    conv_input = jnp.dot(normed, conv_in_weight, preferred_element_type=jnp.float32).astype(jnp.bfloat16)
    gate_outer = jnp.dot(normed, gate_outer_weight, preferred_element_type=jnp.float32).astype(jnp.bfloat16)
    gate_inner = jnp.dot(normed, gate_inner_weight, preferred_element_type=jnp.float32).astype(jnp.bfloat16)
    gated = gate_inner.astype(jnp.float32) * conv_input.astype(jnp.float32)
    gated = gated.reshape(TOKENS // SEQ, SEQ, CONV)
    padded = jnp.pad(gated, ((0, 0), (TAPS - 1, 0), (0, 0)))
    convolved = conv_taps[0] * padded[:, 0:SEQ] + conv_taps[1] * padded[:, 1:SEQ + 1] + conv_taps[2] * padded[:, 2:SEQ + 2]
    convolved = convolved.reshape(TOKENS, CONV)
    mixed = (gate_outer.astype(jnp.float32) * convolved).astype(jnp.bfloat16)
    resid = (tokens.astype(jnp.float32) + block_sum(mixed, out_weight, CONV_DEV)).astype(jnp.bfloat16)
    normed_ff = rms_scale(resid, ff_gain)
    preact = jnp.dot(normed_ff, up_weight, preferred_element_type=jnp.float32)
    hidden = jnp.square(jax.nn.relu(preact)).astype(jnp.bfloat16)
    return (resid.astype(jnp.float32) + block_sum(hidden, down_weight, FF_DEV)).astype(jnp.bfloat16)
```

```python
import jax
import jax.numpy as jnp
from jax import lax
from jax.sharding import Mesh, PartitionSpec as P

eps = 1e-06


def rms_scale(values, gain):
    widened = values.astype(jnp.float32)
    inverse = lax.rsqrt(jnp.mean(widened * widened, axis=-1, keepdims=True) + eps)
    return (widened * inverse * gain).astype(jnp.bfloat16)


GROUP = ("rep", "near", "tp")


def gather_rows(block, near):
    rows, width = block.shape[0], block.shape[1] // near
    if near > 1:
        block = lax.all_to_all(
            block.reshape(rows, near, width).transpose(1, 0, 2), "near", 0, 0, tiled=True
        ).reshape(near * rows, width)
    return lax.all_gather(block, "far", axis=0, tiled=True)


def own_part(block, axis, rep):
    size = block.shape[axis] // rep
    return lax.dynamic_slice_in_dim(block, lax.axis_index("rep") * size, size, axis)


def on_device(rep, near, tp, tokens, mix_gain, conv_in, outer, inner, taps, out_w, ff_gain, up_w, down_w):
    seq_rows = tokens.shape[0] * tp
    depth = up_w.shape[0]
    parts = [own_part(w, 1, rep) for w in (conv_in, outer, inner)]
    width = parts[0].shape[1] // near
    trio = jnp.concatenate([p.reshape(depth, near, width) for p in parts], 2).reshape(depth, -1)
    trio = gather_rows(trio, near)
    out_part = own_part(out_w, 0, rep)
    out_part = out_part.reshape(near, width, -1).transpose(1, 0, 2).reshape(width, -1)
    out_full = gather_rows(out_part, near).reshape(-1, width, out_w.shape[1])
    up_full = gather_rows(own_part(up_w, 1, rep), near)
    down_part = own_part(down_w, 0, rep)
    hid = down_part.shape[0] // near
    down_part = down_part.reshape(near, hid, -1).transpose(1, 0, 2).reshape(hid, -1)
    down_full = gather_rows(down_part, near).reshape(-1, hid, down_w.shape[1])

    taps = own_part(taps, 1, rep)
    taps = lax.dynamic_slice_in_dim(taps, lax.axis_index("near") * width, width, 1)

    normed = lax.all_gather(rms_scale(tokens, mix_gain), GROUP, axis=0, tiled=True)
    proj = jnp.dot(normed, trio, preferred_element_type=jnp.float32).astype(jnp.bfloat16)
    proj = proj.astype(jnp.float32).reshape(-1, seq_rows, 3 * width)
    gated = proj[..., 2 * width :] * proj[..., :width]
    padded = jnp.pad(gated, ((0, 0), (2, 0), (0, 0)))
    convolved = sum(taps[k] * padded[:, k : seq_rows + k] for k in range(3))
    mixed = (proj[..., width : 2 * width] * convolved).astype(jnp.bfloat16)
    mixed = mixed.reshape(-1, width)

    def project(lefts, rights):
        whole = rights.transpose(1, 0, 2).reshape(lefts.shape[1], -1)
        partial = jnp.dot(lefts, whole, preferred_element_type=jnp.float32)
        return lax.psum_scatter(
            partial.astype(jnp.bfloat16), GROUP, scatter_dimension=0, tiled=True
        ).astype(jnp.float32)

    resid = (tokens.astype(jnp.float32) + project(mixed, out_full)).astype(jnp.bfloat16)
    normed_ff = lax.all_gather(rms_scale(resid, ff_gain), GROUP, axis=0, tiled=True)
    preact = jnp.dot(normed_ff, up_full, preferred_element_type=jnp.float32)
    hidden = jnp.square(jax.nn.relu(preact)).astype(jnp.bfloat16)
    return (resid.astype(jnp.float32) + project(hidden, down_full)).astype(jnp.bfloat16)


def solution(mesh):
    rep, fs, tp = (mesh.shape[name] for name in ("rep", "fs", "tp"))
    near = 2 if fs % 2 == 0 else 1
    mesh4 = Mesh(mesh.devices.reshape(rep, fs // near, near, tp), ("rep", "far", "near", "tp"))
    fs_axes = ("far", "near")
    rows = P(("rep", "far", "near", "tp"), None)
    in_specs = (
        rows,
        P(),
        P(fs_axes, "tp"),
        P(fs_axes, "tp"),
        P(fs_axes, "tp"),
        P(None, "tp"),
        P("tp", fs_axes),
        P(),
        P(fs_axes, "tp"),
        P("tp", fs_axes),
    )

    def body(*args):
        return on_device(rep, near, tp, *args)

    return jax.shard_map(body, mesh=mesh4, in_specs=in_specs, out_specs=rows, check_vma=False)
```

```python
import functools

import jax
import jax.numpy as jnp
from jax import lax
from jax.experimental import pallas as pl
from jax.experimental.pallas import tpu as pltpu
from jax.sharding import Mesh, PartitionSpec as P

eps = 1e-06


def rms_scale(values, gain):
    widened = values.astype(jnp.float32)
    inverse = lax.rsqrt(jnp.mean(widened * widened, axis=-1, keepdims=True) + eps)
    return (widened * inverse * gain).astype(jnp.bfloat16)


GROUP = ("rep", "near", "tp")


def gather_rows(block, near):
    rows, width = block.shape[0], block.shape[1] // near
    if near > 1:
        block = lax.all_to_all(
            block.reshape(rows, near, width).transpose(1, 0, 2), "near", 0, 0, tiled=True
        ).reshape(near * rows, width)
    return lax.all_gather(block, "far", axis=0, tiled=True)


def own_part(block, axis, rep):
    size = block.shape[axis] // rep
    return lax.dynamic_slice_in_dim(block, lax.axis_index("rep") * size, size, axis)


def on_device(rep, near, tp, tokens, mix_gain, conv_in, outer, inner, taps, out_w, ff_gain, up_w, down_w):
    seq_rows = tokens.shape[0] * tp
    depth = up_w.shape[0]
    parts = [own_part(w, 1, rep) for w in (conv_in, outer, inner)]
    width = parts[0].shape[1] // near
    trio = jnp.concatenate([p.reshape(depth, near, width) for p in parts], 2).reshape(depth, -1)
    trio = gather_rows(trio, near)
    out_part = own_part(out_w, 0, rep)
    out_part = out_part.reshape(near, width, -1).transpose(1, 0, 2).reshape(width, -1)
    out_full = gather_rows(out_part, near).reshape(-1, width, out_w.shape[1])
    up_full = gather_rows(own_part(up_w, 1, rep), near)
    down_part = own_part(down_w, 0, rep)
    hid = down_part.shape[0] // near
    down_part = down_part.reshape(near, hid, -1).transpose(1, 0, 2).reshape(hid, -1)
    down_full = gather_rows(down_part, near).reshape(-1, hid, down_w.shape[1])

    taps = own_part(taps, 1, rep)
    taps = lax.dynamic_slice_in_dim(taps, lax.axis_index("near") * width, width, 1)

    normed = lax.all_gather(rms_scale(tokens, mix_gain), GROUP, axis=0, tiled=True)
    proj = jnp.dot(normed, trio, preferred_element_type=jnp.float32).astype(jnp.bfloat16)
    proj = proj.astype(jnp.float32).reshape(-1, seq_rows, 3 * width)
    gated = proj[..., 2 * width :] * proj[..., :width]
    padded = jnp.pad(gated, ((0, 0), (2, 0), (0, 0)))
    convolved = sum(taps[k] * padded[:, k : seq_rows + k] for k in range(3))
    mixed = (proj[..., width : 2 * width] * convolved).astype(jnp.bfloat16)
    mixed = mixed.reshape(-1, width)

    def project(lefts, rights):
        whole = rights.transpose(1, 0, 2).reshape(lefts.shape[1], -1)
        partial = jnp.dot(lefts, whole, preferred_element_type=jnp.float32)
        return lax.psum_scatter(
            partial.astype(jnp.bfloat16), GROUP, scatter_dimension=0, tiled=True
        ).astype(jnp.float32)

    resid = (tokens.astype(jnp.float32) + project(mixed, out_full)).astype(jnp.bfloat16)
    normed_ff = lax.all_gather(rms_scale(resid, ff_gain), GROUP, axis=0, tiled=True)
    preact = jnp.dot(normed_ff, up_full, preferred_element_type=jnp.float32)
    hidden = jnp.square(jax.nn.relu(preact)).astype(jnp.bfloat16)
    return (resid.astype(jnp.float32) + project(hidden, down_full)).astype(jnp.bfloat16)


def visit_order(far):
    return [sorted(range(far), key=lambda s: (abs(s - z), s)) for z in range(far)]


def layer_kernel(
    far,
    tok_ref, mix_gain_ref, conv_ref, outer_ref, inner_ref, taps_ref, outw_ref, ff_gain_ref, upw_ref, dnw_ref,
    o_ref,
    trio, outb, upb, dnb, stage, toks, toks_ff, part, sib, rsend, rrecv, part_ff, sib_ff, rsend_ff, rrecv_ff,
    hidden, resid,
    local_sem, stage_sem, near_send, right_send, left_send, w_recv,
    ag_send, ag_recv, sib_send, sib_recv, rs_send, rs_recv,
):
    r, z, y, t = (lax.axis_index(name) for name in ("rep", "far", "near", "tp"))
    m = r * 2 + y
    rows = tok_ref.shape[0]
    seq = 2 * rows
    width = trio.shape[1] // 3
    depth, hid = upw_ref.shape[0], upb.shape[1]
    cols = dnw_ref.shape[1]
    bf16, f32 = jnp.bfloat16, jnp.float32

    def al(v, n):
        return pl.multiple_of(v, n)

    def push(a, b, s, q, where):
        return pltpu.make_async_remote_copy(
            src_ref=a, dst_ref=b, send_sem=s, recv_sem=q, device_id=where, device_id_type=pl.DeviceIdType.MESH
        )

    def chip(c):
        return (lax.div(c, 2), z, lax.rem(c, 2), t)

    sibling = (r, z, y, 1 - t)
    beside = (r, z, 1 - y, t)

    def place(k, zs, ys):
        p = zs * 2 + ys
        if k == 0:
            return trio.at[pl.ds(al(p * depth, depth), depth), :]
        if k == 1:
            return outb.at[:, pl.ds(al(p * cols, cols), cols)]
        if k == 2:
            return upb.at[pl.ds(al(p * depth, depth), depth), :]
        return dnb.at[:, pl.ds(al(p * cols, cols), cols)]

    def share(k, ys):
        q = r * 2 + ys
        if k == 1:
            return outw_ref.at[pl.ds(al(q * width, width), width), :]
        if k == 2:
            return upw_ref.at[:, pl.ds(al(q * hid, hid), hid)]
        return dnw_ref.at[pl.ds(al(q * hid, hid), hid), :]

    trio_in = (conv_ref, outer_ref, inner_ref)

    def trio_copies(dst, ys, sems):
        q = r * 2 + ys
        return [
            pltpu.make_async_copy(
                w.at[:, pl.ds(al(q * width, width), width)],
                dst.at[:, pl.ds(j * width, width)],
                sems.at[j],
            )
            for j, w in enumerate(trio_in)
        ]

    own_trio = trio_copies(place(0, z, y), y, local_sem)
    other_trio = trio_copies(stage, 1 - y, stage_sem)
    own_rest = [None] + [pltpu.make_async_copy(share(k, y), place(k, z, y), local_sem.at[2 + k]) for k in (1, 2, 3)]
    for copy in other_trio + own_trio + own_rest[1:]:
        copy.start()

    def near_copy(k):
        a = stage if k == 0 else share(k, 1 - y)
        return push(a, place(k, z, y), near_send.at[k], w_recv.at[k, z * 2 + y], beside)

    def hop(k, zs, ys, step, sems):
        p = zs * 2 + ys
        at = place(k, zs, ys)
        return push(at, at, sems.at[k, p], w_recv.at[k, p], (r, z + step, y, t))

    order = visit_order(far)

    def nth(j):
        zs = jnp.int32(order[0][j])
        for c in range(1, far):
            zs = jnp.where(z == c, order[c][j], zs)
        return zs

    def send_on(k, zs, ys):
        @pl.when(jnp.logical_and(zs <= z, z + 1 < far))
        def _():
            hop(k, zs, ys, 1, right_send).start()

        @pl.when(jnp.logical_and(zs >= z, z > 0))
        def _():
            hop(k, zs, ys, -1, left_send).start()

    def arrive_own(k):
        for copy in own_trio if k == 0 else [own_rest[k]]:
            copy.wait()
        send_on(k, z, y)

    def arrive_beside(k):
        push(place(k, z, 1 - y), place(k, z, 1 - y), near_send.at[k], w_recv.at[k, z * 2 + 1 - y], beside).wait_recv()
        send_on(k, z, 1 - y)

    def arrive(k, j):
        zs = nth(j)
        for ys in (y, 1 - y):
            push(
                place(k, zs, ys), place(k, zs, ys), near_send.at[k], w_recv.at[k, zs * 2 + ys], beside
            ).wait_recv()
            send_on(k, zs, ys)
        return zs

    def norm(values, gain_ref):
        inverse = lax.rsqrt(jnp.mean(values * values, axis=-1, keepdims=True) + eps)
        return (values * inverse * gain_ref[...]).astype(bf16)

    def slot(buf, c, core):
        return buf.at[pl.ds(al((c * 2 + core) * rows, rows), rows), :]

    def ag_copy(g, buf, i):
        at = slot(buf, m, t)
        where = sibling if i == 3 else chip(lax.rem(m + 1 + i, 4))
        return push(at, at, ag_send.at[g, i], ag_recv.at[g, m * 2 + t], where)

    def ag_relay(g, buf, i):
        c = lax.rem(m + 3 - i, 4)
        at = slot(buf, c, t)
        return push(at, at, ag_send.at[g, 4 + i], ag_recv.at[g, c * 2 + t], sibling)

    def ag_start(g, buf):
        for i in range(4):
            ag_copy(g, buf, i).start()

    def ag_wait(g, buf, c, core):
        at = slot(buf, c, core)
        push(at, at, ag_send.at[g, 0], ag_recv.at[g, c * 2 + core], sibling).wait_recv()

    def ag_finish(g, buf):
        for i in (0, 2, 1):
            ag_wait(g, buf, lax.rem(m + 3 - i, 4), t)
            ag_relay(g, buf, i).start()
        for i in range(4):
            ag_wait(g, buf, lax.rem(m + 3 - i, 4), 1 - t)

    for copy in other_trio:
        copy.wait()
    near_copy(0).start()
    near_copy(1).start()
    arrive_own(0)
    arrive_own(1)
    toks[pl.ds(al((m * 2 + t) * rows, rows), rows), :] = norm(tok_ref[...].astype(f32), mix_gain_ref)
    ag_start(0, toks)
    near_copy(2).start()
    near_copy(3).start()
    for k in (0, 1):
        arrive_beside(k)
    for j in range(1, far):
        for k in (0, 1):
            arrive(k, j)
        if j == 1:
            ag_finish(0, toks)
    arrive_own(2)
    arrive_beside(2)

    mix_cols = outb.shape[1]
    q = r * 2 + y
    taps = taps_ref[:, pl.ds(al(q * width, width), width)]

    def sib_copy(g, n, s, buf, land, lo, size):
        at = buf.at[pl.ds(al(s * seq + (1 - t) * rows, rows), rows), pl.ds(lo, size)]
        to = land.at[pl.ds(al(s * rows, rows), rows), pl.ds(lo, size)]
        return push(at, to, sib_send.at[n, s], sib_recv.at[n, s], sibling)

    def rs_copy(n, i, send, land, lo, size):
        at = send.at[i, :, pl.ds(lo, size)]
        return push(at, land.at[i, :, pl.ds(lo, size)], rs_send.at[n, i], rs_recv.at[n, i], chip(lax.rem(m + 1 + i, 4)))

    def rs_middle(g, n, buf, land, send, rland, lo, size):
        for i in range(4):
            s = lax.rem(m + 1 + i, 4)
            sib_copy(g, n, s, buf, land, lo, size).wait_recv()
            total = (
                buf[pl.ds(al(s * seq + t * rows, rows), rows), pl.ds(lo, size)].astype(f32)
                + land[pl.ds(al(s * rows, rows), rows), pl.ds(lo, size)].astype(f32)
            )
            send[i, :, pl.ds(lo, size)] = total.astype(bf16)
            if i < 3:
                rs_copy(n, i, send, rland, lo, size).start()

    def rs_total(n, send, rland, lo, size):
        total = send[3, :, pl.ds(lo, size)].astype(f32)
        for i in range(3):
            rs_copy(n, i, send, rland, lo, size).wait_recv()
            total = total + rland[i, :, pl.ds(lo, size)].astype(f32)
        return total

    @pl.loop(0, 4)
    def _(i):
        s = lax.rem(m + 1 + i, 4)
        x = toks[pl.ds(al(s * seq, seq), seq), :]
        proj = jnp.dot(x, trio[...], preferred_element_type=f32).astype(bf16).astype(f32)
        gated = proj[:, 2 * width :] * proj[:, :width]
        row = lax.broadcasted_iota(jnp.int32, gated.shape, 0)
        back1 = jnp.where(row < 1, 0.0, pltpu.roll(gated, 1, 0))
        back2 = jnp.where(row < 2, 0.0, pltpu.roll(gated, 2, 0))
        convolved = taps[0:1] * back2 + taps[1:2] * back1 + taps[2:3] * gated
        mixed = (proj[:, width : 2 * width] * convolved).astype(bf16)
        for lo in range(0, mix_cols, 1024):
            size = min(1024, mix_cols - lo)
            part[pl.ds(al(s * seq, seq), seq), pl.ds(lo, size)] = jnp.dot(
                mixed, outb[:, pl.ds(lo, size)], preferred_element_type=f32
            ).astype(bf16)
        sib_copy(0, 0, s, part, sib, 0, mix_cols).start()

    rs_middle(0, 0, part, sib, rsend, rrecv, 0, mix_cols)
    arrive(2, 1)
    resid[...] = (tok_ref[...].astype(f32) + rs_total(0, rsend, rrecv, 0, mix_cols)).astype(bf16)
    toks_ff[pl.ds(al((m * 2 + t) * rows, rows), rows), :] = norm(resid[...].astype(f32), ff_gain_ref)
    ag_start(1, toks_ff)
    for j in range(2, far):
        arrive(2, j)
        if j == 2:
            ag_finish(1, toks_ff)
    if far < 3:
        ag_finish(1, toks_ff)
    arrive_own(3)
    arrive_beside(3)

    @pl.loop(0, 4)
    def _(s):
        x = toks_ff[pl.ds(al(s * seq, seq), seq), :]
        half = hid // 2
        for lo in (0, half):
            act = jnp.dot(x, upb[:, pl.ds(lo, half)], preferred_element_type=f32)
            hidden[pl.ds(al(s * seq, seq), seq), pl.ds(lo, half)] = jnp.square(jnp.maximum(act, 0.0)).astype(bf16)

    group = 2 * cols

    def down(zs):
        lo = al(zs * group, group)

        @pl.loop(0, 4)
        def _(i):
            s = lax.rem(m + 1 + i, 4)
            part_ff[pl.ds(al(s * seq, seq), seq), pl.ds(lo, group)] = jnp.dot(
                hidden[pl.ds(al(s * seq, seq), seq), :], dnb[:, pl.ds(lo, group)], preferred_element_type=f32
            ).astype(bf16)
            sib_copy(1, 1 + zs, s, part_ff, sib_ff, lo, group).start()

        rs_middle(1, 1 + zs, part_ff, sib_ff, rsend_ff, rrecv_ff, lo, group)

    down(z)
    for j in range(1, far):
        down(arrive(3, j))
    for j in range(far):
        zs = nth(j)
        lo = al(zs * group, group)
        total = rs_total(1 + zs, rsend_ff, rrecv_ff, lo, group)
        o_ref[:, pl.ds(lo, group)] = (resid[:, pl.ds(lo, group)].astype(f32) + total).astype(bf16)

    for k in range(4):
        near_copy(k).wait_send()
        for zs in range(far):
            for ys in range(2):
                @pl.when(jnp.logical_and(zs <= z, z + 1 < far))
                def _():
                    hop(k, zs, ys, 1, right_send).wait_send()

                @pl.when(jnp.logical_and(zs >= z, z > 0))
                def _():
                    hop(k, zs, ys, -1, left_send).wait_send()
    for g, buf in ((0, toks), (1, toks_ff)):
        for i in range(4):
            ag_copy(g, buf, i).wait_send()
        for i in range(3):
            ag_relay(g, buf, i).wait_send()
    for s in range(4):
        sib_copy(0, 0, s, part, sib, 0, mix_cols).wait_send()
        for zs in range(far):
            sib_copy(1, 1 + zs, s, part_ff, sib_ff, zs * group, group).wait_send()
    for i in range(3):
        rs_copy(0, i, rsend, rrecv, 0, mix_cols).wait_send()
        for zs in range(far):
            rs_copy(1 + zs, i, rsend_ff, rrecv_ff, zs * group, group).wait_send()


def fused_layer(far, tokens, mix_gain, conv_in, outer, inner, taps, out_w, ff_gain, up_w, down_w):
    bf16 = jnp.bfloat16
    rows, feat = tokens.shape
    depth, cols = up_w.shape[0], down_w.shape[1]
    width, hid = conv_in.shape[1] // 4, up_w.shape[1] // 4
    whole = 8 * rows
    vmem = pl.BlockSpec(memory_space=pltpu.VMEM)
    hbm = pl.BlockSpec(memory_space=pl.ANY)
    dma = pltpu.SemaphoreType.DMA
    block = [
        pltpu.VMEM((whole, feat), bf16),
        pltpu.VMEM((4 * rows, feat), bf16),
        pltpu.VMEM((4, rows, feat), bf16),
        pltpu.VMEM((3, rows, feat), bf16),
    ]
    return pl.pallas_call(
        functools.partial(layer_kernel, far),
        out_shape=jax.ShapeDtypeStruct((rows, feat), bf16),
        in_specs=[vmem, vmem, hbm, hbm, hbm, vmem, hbm, vmem, hbm, hbm],
        out_specs=vmem,
        scratch_shapes=[
            pltpu.VMEM((far * 2 * depth, 3 * width), bf16),
            pltpu.VMEM((width, far * 2 * cols), bf16),
            pltpu.VMEM((far * 2 * depth, hid), bf16),
            pltpu.VMEM((hid, far * 2 * cols), bf16),
            pltpu.VMEM((depth, 3 * width), bf16),
            pltpu.VMEM((whole, feat), bf16),
            pltpu.VMEM((whole, feat), bf16),
            *block,
            *block,
            pltpu.VMEM((whole, hid), bf16),
            pltpu.VMEM((rows, feat), bf16),
            dma((6,)),
            dma((3,)),
            dma((4,)),
            dma((4, far * 2)),
            dma((4, far * 2)),
            dma((4, far * 2)),
            dma((2, 7)),
            dma((2, 8)),
            dma((1 + far, 4)),
            dma((1 + far, 4)),
            dma((1 + far, 3)),
            dma((1 + far, 3)),
        ],
        compiler_params=pltpu.CompilerParams(has_side_effects=True, vmem_limit_bytes=60 * 2**20),
    )(tokens, mix_gain[None], conv_in, outer, inner, taps, out_w, ff_gain[None], up_w, down_w)


def solution(mesh):
    rep, fs, tp = (mesh.shape[name] for name in ("rep", "fs", "tp"))
    near = 2 if fs % 2 == 0 else 1
    mesh4 = Mesh(mesh.devices.reshape(rep, fs // near, near, tp), ("rep", "far", "near", "tp"))
    fs_axes = ("far", "near")
    rows = P(("rep", "far", "near", "tp"), None)
    in_specs = (
        rows,
        P(),
        P(fs_axes, "tp"),
        P(fs_axes, "tp"),
        P(fs_axes, "tp"),
        P(None, "tp"),
        P("tp", fs_axes),
        P(),
        P(fs_axes, "tp"),
        P("tp", fs_axes),
    )

    def body(*args):
        if rep == 2 and near == 2 and tp == 2:
            return fused_layer(fs // near, *args)
        return on_device(rep, near, tp, *args)

    return jax.shard_map(body, mesh=mesh4, in_specs=in_specs, out_specs=rows, check_vma=False)
```

```python
import functools

import jax
import jax.numpy as jnp
from jax import lax
from jax.experimental import pallas as pl
from jax.experimental.pallas import tpu as pltpu
from jax.sharding import Mesh, PartitionSpec as P

eps = 1e-06


def rms_scale(values, gain):
    widened = values.astype(jnp.float32)
    inverse = lax.rsqrt(jnp.mean(widened * widened, axis=-1, keepdims=True) + eps)
    return (widened * inverse * gain).astype(jnp.bfloat16)


GROUP = ("rep", "near", "tp")


def gather_rows(block, near):
    rows, width = block.shape[0], block.shape[1] // near
    if near > 1:
        block = lax.all_to_all(
            block.reshape(rows, near, width).transpose(1, 0, 2), "near", 0, 0, tiled=True
        ).reshape(near * rows, width)
    return lax.all_gather(block, "far", axis=0, tiled=True)


def own_part(block, axis, rep):
    size = block.shape[axis] // rep
    return lax.dynamic_slice_in_dim(block, lax.axis_index("rep") * size, size, axis)


def on_device(rep, near, tp, tokens, mix_gain, conv_in, outer, inner, taps, out_w, ff_gain, up_w, down_w):
    seq_rows = tokens.shape[0] * tp
    depth = up_w.shape[0]
    parts = [own_part(w, 1, rep) for w in (conv_in, outer, inner)]
    width = parts[0].shape[1] // near
    trio = jnp.concatenate([p.reshape(depth, near, width) for p in parts], 2).reshape(depth, -1)
    trio = gather_rows(trio, near)
    out_part = own_part(out_w, 0, rep)
    out_part = out_part.reshape(near, width, -1).transpose(1, 0, 2).reshape(width, -1)
    out_full = gather_rows(out_part, near).reshape(-1, width, out_w.shape[1])
    up_full = gather_rows(own_part(up_w, 1, rep), near)
    down_part = own_part(down_w, 0, rep)
    hid = down_part.shape[0] // near
    down_part = down_part.reshape(near, hid, -1).transpose(1, 0, 2).reshape(hid, -1)
    down_full = gather_rows(down_part, near).reshape(-1, hid, down_w.shape[1])

    taps = own_part(taps, 1, rep)
    taps = lax.dynamic_slice_in_dim(taps, lax.axis_index("near") * width, width, 1)

    normed = lax.all_gather(rms_scale(tokens, mix_gain), GROUP, axis=0, tiled=True)
    proj = jnp.dot(normed, trio, preferred_element_type=jnp.float32).astype(jnp.bfloat16)
    proj = proj.astype(jnp.float32).reshape(-1, seq_rows, 3 * width)
    gated = proj[..., 2 * width :] * proj[..., :width]
    padded = jnp.pad(gated, ((0, 0), (2, 0), (0, 0)))
    convolved = sum(taps[k] * padded[:, k : seq_rows + k] for k in range(3))
    mixed = (proj[..., width : 2 * width] * convolved).astype(jnp.bfloat16)
    mixed = mixed.reshape(-1, width)

    def project(lefts, rights):
        whole = rights.transpose(1, 0, 2).reshape(lefts.shape[1], -1)
        partial = jnp.dot(lefts, whole, preferred_element_type=jnp.float32)
        return lax.psum_scatter(
            partial.astype(jnp.bfloat16), GROUP, scatter_dimension=0, tiled=True
        ).astype(jnp.float32)

    resid = (tokens.astype(jnp.float32) + project(mixed, out_full)).astype(jnp.bfloat16)
    normed_ff = lax.all_gather(rms_scale(resid, ff_gain), GROUP, axis=0, tiled=True)
    preact = jnp.dot(normed_ff, up_full, preferred_element_type=jnp.float32)
    hidden = jnp.square(jax.nn.relu(preact)).astype(jnp.bfloat16)
    return (resid.astype(jnp.float32) + project(hidden, down_full)).astype(jnp.bfloat16)


def visit_order(far):
    return [sorted(range(far), key=lambda s: (abs(s - z), s)) for z in range(far)]


def layer_kernel(
    far,
    tok_ref, mix_gain_ref, conv_ref, outer_ref, inner_ref, taps_ref, outw_ref, ff_gain_ref, upw_ref, dnw_ref,
    o_ref,
    trio, outb, upb, dnb, stage, toks, toks_ff, part, sib, rsend, rrecv, part_ff, sib_ff, rsend_ff, rrecv_ff,
    hidden, resid,
    local_sem, stage_sem, near_send, right_send, left_send, w_recv,
    ag_send, ag_recv, sib_send, sib_recv, rs_send, rs_recv,
):
    r, z, y, t = (lax.axis_index(name) for name in ("rep", "far", "near", "tp"))
    m = r * 2 + y
    rows = tok_ref.shape[0]
    seq = 2 * rows
    width = trio.shape[1] // 3
    depth, hid = upw_ref.shape[0], upb.shape[1]
    cols = dnw_ref.shape[1]
    bf16, f32 = jnp.bfloat16, jnp.float32

    def al(v, n):
        return pl.multiple_of(v, n)

    def push(a, b, s, q, where):
        return pltpu.make_async_remote_copy(
            src_ref=a, dst_ref=b, send_sem=s, recv_sem=q, device_id=where, device_id_type=pl.DeviceIdType.MESH
        )

    def chip(c):
        return (lax.div(c, 2), z, lax.rem(c, 2), t)

    sibling = (r, z, y, 1 - t)
    beside = (r, z, 1 - y, t)

    def place(k, zs, ys):
        p = zs * 2 + ys
        if k == 0:
            return trio.at[pl.ds(al(p * depth, depth), depth), :]
        if k == 1:
            return outb.at[:, pl.ds(al(p * cols, cols), cols)]
        if k == 2:
            return upb.at[pl.ds(al(p * depth, depth), depth), :]
        return dnb.at[:, pl.ds(al(p * cols, cols), cols)]

    def share(k, ys):
        q = r * 2 + ys
        if k == 1:
            return outw_ref.at[pl.ds(al(q * width, width), width), :]
        if k == 2:
            return upw_ref.at[:, pl.ds(al(q * hid, hid), hid)]
        return dnw_ref.at[pl.ds(al(q * hid, hid), hid), :]

    trio_in = (conv_ref, outer_ref, inner_ref)

    def trio_copies(dst, ys, sems):
        q = r * 2 + ys
        return [
            pltpu.make_async_copy(
                w.at[:, pl.ds(al(q * width, width), width)],
                dst.at[:, pl.ds(j * width, width)],
                sems.at[j],
            )
            for j, w in enumerate(trio_in)
        ]

    own_trio = trio_copies(place(0, z, y), y, local_sem)
    other_trio = trio_copies(stage, 1 - y, stage_sem)
    own_rest = [None] + [pltpu.make_async_copy(share(k, y), place(k, z, y), local_sem.at[2 + k]) for k in (1, 2, 3)]
    for copy in other_trio + own_trio + own_rest[1:]:
        copy.start()

    def near_copy(k):
        a = stage if k == 0 else share(k, 1 - y)
        return push(a, place(k, z, y), near_send.at[k], w_recv.at[k, z * 2 + y], beside)

    def hop(k, zs, ys, step, sems):
        p = zs * 2 + ys
        at = place(k, zs, ys)
        return push(at, at, sems.at[k, p], w_recv.at[k, p], (r, z + step, y, t))

    order = visit_order(far)

    def nth(j):
        zs = jnp.int32(order[0][j])
        for c in range(1, far):
            zs = jnp.where(z == c, order[c][j], zs)
        return zs

    def send_on(k, zs, ys):
        @pl.when(jnp.logical_and(zs <= z, z + 1 < far))
        def _():
            hop(k, zs, ys, 1, right_send).start()

        @pl.when(jnp.logical_and(zs >= z, z > 0))
        def _():
            hop(k, zs, ys, -1, left_send).start()

    def arrive_own(k):
        for copy in own_trio if k == 0 else [own_rest[k]]:
            copy.wait()
        send_on(k, z, y)

    def arrive_beside(k):
        push(place(k, z, 1 - y), place(k, z, 1 - y), near_send.at[k], w_recv.at[k, z * 2 + 1 - y], beside).wait_recv()
        send_on(k, z, 1 - y)

    def arrive(k, j):
        zs = nth(j)
        for ys in (y, 1 - y):
            push(
                place(k, zs, ys), place(k, zs, ys), near_send.at[k], w_recv.at[k, zs * 2 + ys], beside
            ).wait_recv()
            send_on(k, zs, ys)
        return zs

    def norm(values, gain_ref):
        inverse = lax.rsqrt(jnp.mean(values * values, axis=-1, keepdims=True) + eps)
        return (values * inverse * gain_ref[...]).astype(bf16)

    def slot(buf, c, core):
        return buf.at[pl.ds(al((c * 2 + core) * rows, rows), rows), :]

    def ag_copy(g, buf, i):
        at = slot(buf, m, t)
        where = sibling if i == 3 else chip(lax.rem(m + 1 + i, 4))
        return push(at, at, ag_send.at[g, i], ag_recv.at[g, m * 2 + t], where)

    def ag_relay(g, buf, i):
        c = lax.rem(m + 3 - i, 4)
        at = slot(buf, c, t)
        return push(at, at, ag_send.at[g, 4 + i], ag_recv.at[g, c * 2 + t], sibling)

    def ag_start(g, buf):
        for i in range(4):
            ag_copy(g, buf, i).start()

    def ag_wait(g, buf, c, core):
        at = slot(buf, c, core)
        push(at, at, ag_send.at[g, 0], ag_recv.at[g, c * 2 + core], sibling).wait_recv()

    def ag_finish(g, buf):
        for i in (0, 2, 1):
            ag_wait(g, buf, lax.rem(m + 3 - i, 4), t)
            ag_relay(g, buf, i).start()
        for i in range(4):
            ag_wait(g, buf, lax.rem(m + 3 - i, 4), 1 - t)

    for copy in other_trio:
        copy.wait()
    near_copy(0).start()
    near_copy(1).start()
    arrive_own(0)
    arrive_own(1)
    toks[pl.ds(al((m * 2 + t) * rows, rows), rows), :] = norm(tok_ref[...].astype(f32), mix_gain_ref)
    ag_start(0, toks)
    near_copy(2).start()
    near_copy(3).start()
    for k in (0, 1):
        arrive_beside(k)
    arrive_own(2)
    arrive_beside(2)
    for j in range(1, far):
        for k in (0, 1):
            arrive(k, j)
        if j == 1:
            ag_finish(0, toks)
    arrive_own(3)
    arrive_beside(3)

    mix_cols = outb.shape[1]
    q = r * 2 + y
    taps = taps_ref[:, pl.ds(al(q * width, width), width)]

    def sib_copy(g, n, s, buf, land, lo, size):
        at = buf.at[pl.ds(al(s * seq + (1 - t) * rows, rows), rows), pl.ds(lo, size)]
        to = land.at[pl.ds(al(s * rows, rows), rows), pl.ds(lo, size)]
        return push(at, to, sib_send.at[n, s], sib_recv.at[n, s], sibling)

    def rs_copy(n, i, send, land, lo, size):
        at = send.at[i, :, pl.ds(lo, size)]
        return push(at, land.at[i, :, pl.ds(lo, size)], rs_send.at[n, i], rs_recv.at[n, i], chip(lax.rem(m + 1 + i, 4)))

    def rs_middle(g, n, buf, land, send, rland, lo, size):
        for i in range(4):
            s = lax.rem(m + 1 + i, 4)
            sib_copy(g, n, s, buf, land, lo, size).wait_recv()
            total = (
                buf[pl.ds(al(s * seq + t * rows, rows), rows), pl.ds(lo, size)].astype(f32)
                + land[pl.ds(al(s * rows, rows), rows), pl.ds(lo, size)].astype(f32)
            )
            send[i, :, pl.ds(lo, size)] = total.astype(bf16)
            if i < 3:
                rs_copy(n, i, send, rland, lo, size).start()

    def rs_total(n, send, rland, lo, size):
        total = send[3, :, pl.ds(lo, size)].astype(f32)
        for i in range(3):
            rs_copy(n, i, send, rland, lo, size).wait_recv()
            total = total + rland[i, :, pl.ds(lo, size)].astype(f32)
        return total

    @pl.loop(0, 4)
    def _(i):
        s = lax.rem(m + 1 + i, 4)
        x = toks[pl.ds(al(s * seq, seq), seq), :]
        proj = jnp.dot(x, trio[...], preferred_element_type=f32).astype(bf16).astype(f32)
        gated = proj[:, 2 * width :] * proj[:, :width]
        row = lax.broadcasted_iota(jnp.int32, gated.shape, 0)
        back1 = jnp.where(row < 1, 0.0, pltpu.roll(gated, 1, 0))
        back2 = jnp.where(row < 2, 0.0, pltpu.roll(gated, 2, 0))
        convolved = taps[0:1] * back2 + taps[1:2] * back1 + taps[2:3] * gated
        mixed = (proj[:, width : 2 * width] * convolved).astype(bf16)
        for lo in range(0, mix_cols, 1024):
            size = min(1024, mix_cols - lo)
            part[pl.ds(al(s * seq, seq), seq), pl.ds(lo, size)] = jnp.dot(
                mixed, outb[:, pl.ds(lo, size)], preferred_element_type=f32
            ).astype(bf16)
        sib_copy(0, 0, s, part, sib, 0, mix_cols).start()

    rs_middle(0, 0, part, sib, rsend, rrecv, 0, mix_cols)
    arrive(2, 1)
    resid[...] = (tok_ref[...].astype(f32) + rs_total(0, rsend, rrecv, 0, mix_cols)).astype(bf16)
    toks_ff[pl.ds(al((m * 2 + t) * rows, rows), rows), :] = norm(resid[...].astype(f32), ff_gain_ref)
    ag_start(1, toks_ff)
    for j in range(2, far):
        arrive(2, j)
        if j == 2:
            ag_finish(1, toks_ff)
    if far < 3:
        ag_finish(1, toks_ff)

    @pl.loop(0, 4)
    def _(s):
        x = toks_ff[pl.ds(al(s * seq, seq), seq), :]
        half = hid // 2
        for lo in (0, half):
            act = jnp.dot(x, upb[:, pl.ds(lo, half)], preferred_element_type=f32)
            hidden[pl.ds(al(s * seq, seq), seq), pl.ds(lo, half)] = jnp.square(jnp.maximum(act, 0.0)).astype(bf16)

    group = 2 * cols

    def down(zs):
        lo = al(zs * group, group)

        @pl.loop(0, 4)
        def _(i):
            s = lax.rem(m + 1 + i, 4)
            part_ff[pl.ds(al(s * seq, seq), seq), pl.ds(lo, group)] = jnp.dot(
                hidden[pl.ds(al(s * seq, seq), seq), :], dnb[:, pl.ds(lo, group)], preferred_element_type=f32
            ).astype(bf16)
            sib_copy(1, 1 + zs, s, part_ff, sib_ff, lo, group).start()

        rs_middle(1, 1 + zs, part_ff, sib_ff, rsend_ff, rrecv_ff, lo, group)

    down(z)
    for j in range(1, far):
        down(arrive(3, j))
    for j in range(far):
        zs = nth(j)
        lo = al(zs * group, group)
        total = rs_total(1 + zs, rsend_ff, rrecv_ff, lo, group)
        o_ref[:, pl.ds(lo, group)] = (resid[:, pl.ds(lo, group)].astype(f32) + total).astype(bf16)

    for k in range(4):
        near_copy(k).wait_send()
        for zs in range(far):
            for ys in range(2):
                @pl.when(jnp.logical_and(zs <= z, z + 1 < far))
                def _():
                    hop(k, zs, ys, 1, right_send).wait_send()

                @pl.when(jnp.logical_and(zs >= z, z > 0))
                def _():
                    hop(k, zs, ys, -1, left_send).wait_send()
    for g, buf in ((0, toks), (1, toks_ff)):
        for i in range(4):
            ag_copy(g, buf, i).wait_send()
        for i in range(3):
            ag_relay(g, buf, i).wait_send()
    for s in range(4):
        sib_copy(0, 0, s, part, sib, 0, mix_cols).wait_send()
        for zs in range(far):
            sib_copy(1, 1 + zs, s, part_ff, sib_ff, zs * group, group).wait_send()
    for i in range(3):
        rs_copy(0, i, rsend, rrecv, 0, mix_cols).wait_send()
        for zs in range(far):
            rs_copy(1 + zs, i, rsend_ff, rrecv_ff, zs * group, group).wait_send()


def fused_layer(far, tokens, mix_gain, conv_in, outer, inner, taps, out_w, ff_gain, up_w, down_w):
    bf16 = jnp.bfloat16
    rows, feat = tokens.shape
    depth, cols = up_w.shape[0], down_w.shape[1]
    width, hid = conv_in.shape[1] // 4, up_w.shape[1] // 4
    whole = 8 * rows
    vmem = pl.BlockSpec(memory_space=pltpu.VMEM)
    hbm = pl.BlockSpec(memory_space=pl.ANY)
    dma = pltpu.SemaphoreType.DMA
    block = [
        pltpu.VMEM((whole, feat), bf16),
        pltpu.VMEM((4 * rows, feat), bf16),
        pltpu.VMEM((4, rows, feat), bf16),
        pltpu.VMEM((3, rows, feat), bf16),
    ]
    return pl.pallas_call(
        functools.partial(layer_kernel, far),
        out_shape=jax.ShapeDtypeStruct((rows, feat), bf16),
        in_specs=[vmem, vmem, hbm, hbm, hbm, vmem, hbm, vmem, hbm, hbm],
        out_specs=vmem,
        scratch_shapes=[
            pltpu.VMEM((far * 2 * depth, 3 * width), bf16),
            pltpu.VMEM((width, far * 2 * cols), bf16),
            pltpu.VMEM((far * 2 * depth, hid), bf16),
            pltpu.VMEM((hid, far * 2 * cols), bf16),
            pltpu.VMEM((depth, 3 * width), bf16),
            pltpu.VMEM((whole, feat), bf16),
            pltpu.VMEM((whole, feat), bf16),
            *block,
            *block,
            pltpu.VMEM((whole, hid), bf16),
            pltpu.VMEM((rows, feat), bf16),
            dma((6,)),
            dma((3,)),
            dma((4,)),
            dma((4, far * 2)),
            dma((4, far * 2)),
            dma((4, far * 2)),
            dma((2, 7)),
            dma((2, 8)),
            dma((1 + far, 4)),
            dma((1 + far, 4)),
            dma((1 + far, 3)),
            dma((1 + far, 3)),
        ],
        compiler_params=pltpu.CompilerParams(has_side_effects=True, vmem_limit_bytes=60 * 2**20),
    )(tokens, mix_gain[None], conv_in, outer, inner, taps, out_w, ff_gain[None], up_w, down_w)


def solution(mesh):
    rep, fs, tp = (mesh.shape[name] for name in ("rep", "fs", "tp"))
    near = 2 if fs % 2 == 0 else 1
    mesh4 = Mesh(mesh.devices.reshape(rep, fs // near, near, tp), ("rep", "far", "near", "tp"))
    fs_axes = ("far", "near")
    rows = P(("rep", "far", "near", "tp"), None)
    in_specs = (
        rows,
        P(),
        P(fs_axes, "tp"),
        P(fs_axes, "tp"),
        P(fs_axes, "tp"),
        P(None, "tp"),
        P("tp", fs_axes),
        P(),
        P(fs_axes, "tp"),
        P("tp", fs_axes),
    )

    def body(*args):
        if rep == 2 and near == 2 and tp == 2:
            return fused_layer(fs // near, *args)
        return on_device(rep, near, tp, *args)

    return jax.shard_map(body, mesh=mesh4, in_specs=in_specs, out_specs=rows, check_vma=False)
```
